32 devices in a mesh: ep: 4 (over z), tp: 8 (over y, x, core).
Axes of the slice: x: 2, y: 2, z: 4, core: 2. Of those that a mesh axis runs over, the one named last changes fastest.
Arguments:
- tokens: bfloat16 [512, 2048], P('ep', 'tp'), may hold values from -6 to 6
- out_grad: bfloat16 [512, 2048], P('ep', 'tp'), may hold values from -6 to 6
- routes: int32 [512, 2], P('ep'), may hold values from 0 to 3, all different within a row; in each aligned block of 128 rows (0 to 127, 128 to 255, ...) at most 96 rows name the same one
- gates: float32 [512, 2], P('ep'), may hold values from 0.1 to 0.9
- gate_weight: bfloat16 [4, 2048, 5632], P('ep', None, 'tp'), may hold values from -0.125 to 0.125
- up_weight: bfloat16 [4, 2048, 5632], P('ep', None, 'tp'), may hold values from -0.125 to 0.125
- down_weight: bfloat16 [4, 5632, 2048], P('ep', 'tp'), may hold values from -0.078125 to 0.078125
Outputs:
- tokens_grad: bfloat16 [512, 2048], P('ep', 'tp')
- gates_grad: float32 [512, 2], P(('ep', 'tp'))
- gate_weight_grad: bfloat16 [4, 2048, 5632], P('ep', None, 'tp')
- up_weight_grad: bfloat16 [4, 2048, 5632], P('ep', None, 'tp')
- down_weight_grad: bfloat16 [4, 5632, 2048], P('ep', 'tp')
The draws below stay inside these ranges and needn't reach their ends.
Inputs may be any that keep to these rules, and one draw needn't show every extreme that they name: `routes`: the 2 experts of a token differ. In each aligned block of 128 rows (the tokens of one index of ep) no expert is named by more than 96 rows, a bound that some block reaches.
All inputs are finite; a program needn't handle non-finite values.
Results may differ from the reference program's by a relative error of at most 0.029.
Values may be sent and summed in bfloat16 or wider, within the bound.
A program may use at most 64 MiB of HBM per device.

```python
import math
import jax
import jax.numpy as jnp
import numpy as np
from jax import lax

D = 2048
FF = 5632
TOPK = 2
TOK_DEV = 128
EXPERTS = 4
CAP = 96
TOKENS = 512
N_EP = 4
N_TP = 8


def block_scale(stream_key, dims, split, least, top_value):
    gain = 1.0
    for dim, parts in split:
        steps = jax.random.uniform(jax.random.fold_in(jax.random.fold_in(stream_key, 6), dim), (parts,), jnp.float32, least / len(split), top_value / len(split))
        gain = gain * jnp.repeat(jnp.exp(steps), dims[dim] // parts).reshape((-1,) + (1,) * (len(dims) - 1 - dim))
    return gain


def routed_block(own_key, own, number, rows, count, top, reach, slope):
    ranking = jax.random.permutation(own_key, count)
    crowded, ordinary = portions_of(count, rows * top, reach, slope, True), portions_of(count, rows * top, reach, slope, False)
    places = jnp.arange(count)

    def named(tallies, rotation):
        used = int((tallies > 0).sum())
        fixed = max(1, used // 4)
        moved = fixed + (places - fixed + rotation * (used - fixed)) % max(1, count - fixed)
        return jnp.zeros((count,), jnp.int32).at[ranking[jnp.where(places < fixed, places, moved)]].set(jnp.asarray(tallies, jnp.int32))

    tallies = jnp.where(number % 4 == 0, named(crowded, number // 4), named(ordinary, number - number // 4 - 1))
    mixed = jax.random.permutation(jax.random.fold_in(own, 3), count)
    source_of, taker = mixed[0:count // 2 * 2:2], mixed[1:count // 2 * 2:2]
    room = jnp.minimum(tallies[source_of] - 1, reach - tallies[taker]) // 2
    room = jnp.where((source_of == ranking[0]) | (taker == ranking[0]) | (tallies[taker] == 0), 0, jnp.maximum(room, 0))
    moved = jax.random.randint(jax.random.fold_in(own, 4), (count // 2,), 0, 1 << 20) % (room + 1)
    tallies = tallies.at[source_of].add(-moved).at[taker].add(moved)
    items = jnp.searchsorted(jnp.cumsum(tallies), jnp.arange(rows * top), side="right").astype(jnp.int32)
    grid = items.reshape(top, rows).T
    grid = grid[jax.random.permutation(jax.random.fold_in(own, 1), rows)]
    rotation = jax.random.randint(jax.random.fold_in(own, 2), (rows, 1), 0, top)
    return jnp.take_along_axis(grid, (jnp.arange(top)[None, :] + rotation) % top, axis=1)


def portions_of(count, total, bound, slope, full):
    portions = [(1 << 20) // math.isqrt(rank ** slope) + 1 for rank in range(1, count + 1)]
    largest = bound if full else min(bound, max(-(-total // count), total * portions[0] // sum(portions)))
    least = 1 if total - largest >= count - 1 else 0
    holding, surplus = [largest] + [least] * (count - 1), total - largest - least * (count - 1)
    while surplus > 0:
        free = [i for i in range(1, count) if holding[i] < largest] or [i for i in range(1, count) if holding[i] < bound]
        pool, left = sum([portions[i] for i in free]), surplus
        for i in free:
            addition = min(bound - holding[i], max(1, left * portions[i] // pool), surplus)
            holding[i] = holding[i] + addition
            surplus = surplus - addition
    return np.array(holding)


def scatter_about(stream_key, extent, deviation, most, cuts=(), held_as=jnp.bfloat16):
    loudness = block_scale(stream_key, extent, cuts, -0.22, 0.18) if cuts else 1.0
    entries = jax.random.normal(stream_key, extent, jnp.float32) * deviation * loudness
    return jnp.minimum(jnp.maximum(entries, -most), most).astype(held_as)


def setup_inputs(seed: int = 0) -> dict:
    arg_keys = jax.random.split(jax.random.key(seed), 8)
    tokens = scatter_about(arg_keys[0], (TOKENS, D), 1.0, 6.0, ((0, 4), (1, 8)))
    out_grad = scatter_about(arg_keys[1], (TOKENS, D), 1.0, 6.0, ((0, 4), (1, 8)))
    routes_keys = jax.random.split(jax.random.fold_in(arg_keys[2], 1), TOKENS // TOK_DEV)
    routes_turns = jax.random.permutation(jax.random.fold_in(arg_keys[2], 3), TOKENS // TOK_DEV)
    routes = jax.vmap(lambda own, number: routed_block(jax.random.fold_in(arg_keys[2], 2), own, number, TOK_DEV, EXPERTS, TOPK, CAP, 2))(routes_keys, routes_turns).reshape((TOKENS, TOPK))
    gates = jnp.clip(0.1 + 0.79999997 * jax.random.uniform(arg_keys[3], (TOKENS, TOPK), jnp.float32) ** block_scale(arg_keys[3], (TOKENS, TOPK), ((0, 4),), -0.2, 0.2), 0.1, 0.9)
    gate_weight = scatter_about(arg_keys[4], (EXPERTS, D, FF), D ** -0.5, 0.125, ((0, 4), (2, 8)))
    up_weight = scatter_about(arg_keys[5], (EXPERTS, D, FF), D ** -0.5, 0.125, ((0, 4), (2, 8)))
    down_weight = scatter_about(arg_keys[6], (EXPERTS, FF, D), FF ** -0.5, 0.078125, ((0, 4), (1, 8)))
    return {"tokens": tokens, "out_grad": out_grad, "routes": routes, "gates": gates, "gate_weight": gate_weight, "up_weight": up_weight, "down_weight": down_weight}


def expert_grads(rows, cotan, w_gate, w_up, w_down):
    pre_gate = jnp.dot(rows, w_gate, preferred_element_type=jnp.float32)
    pre_up = jnp.dot(rows, w_up, preferred_element_type=jnp.float32)
    activated = jax.nn.silu(pre_gate)
    hidden = (activated * pre_up).astype(jnp.bfloat16)
    hid_grad = jnp.dot(cotan, w_down.T, preferred_element_type=jnp.float32)
    sigmoid_gate = jax.nn.sigmoid(pre_gate)
    gate_part = (hid_grad * pre_up * sigmoid_gate * (1.0 + pre_gate * (1.0 - sigmoid_gate))).astype(jnp.bfloat16)
    up_part = (hid_grad * activated).astype(jnp.bfloat16)
    slot_dots = jnp.sum(hidden.astype(jnp.float32) * hid_grad, axis=1)
    down_grad = jnp.dot(hidden.T, cotan, preferred_element_type=jnp.float32).astype(jnp.bfloat16)
    gate_grad = jnp.dot(rows.T, gate_part, preferred_element_type=jnp.float32).astype(jnp.bfloat16)
    up_grad = jnp.dot(rows.T, up_part, preferred_element_type=jnp.float32).astype(jnp.bfloat16)
    return gate_part, up_part, slot_dots, gate_grad, up_grad, down_grad


def reference(tokens, out_grad, routes, gates, gate_weight, up_weight, down_weight):
    slot_count = TOKENS * TOPK
    flat = jnp.arange(slot_count, dtype=jnp.int32)
    token_of = (flat // TOPK).astype(jnp.int32)
    flat_expert = routes.reshape(-1).astype(jnp.int32)
    onehot = (flat_expert[:, None] == jnp.arange(EXPERTS, dtype=jnp.int32)[None, :]).astype(jnp.int32)
    blocks = onehot.reshape(N_EP, TOK_DEV * TOPK, EXPERTS)
    before = jnp.cumsum(blocks, axis=1) - blocks
    slot_rank = jnp.sum(before * blocks, axis=2).reshape(-1)
    source = (flat // (TOK_DEV * TOPK)).astype(jnp.int32)
    slot_dest = (flat_expert * (N_EP * CAP) + source * CAP + slot_rank).astype(jnp.int32)
    owner = jnp.full((EXPERTS * N_EP * CAP,), slot_count, jnp.int32).at[slot_dest].set(flat)
    owner = owner.reshape(EXPERTS, N_EP * CAP)
    zero_row = jnp.zeros((1, D), jnp.bfloat16)
    row_table = jnp.concatenate([tokens[token_of], zero_row], axis=0)
    scaled = (gates.reshape(-1)[:, None] * out_grad[token_of].astype(jnp.float32)).astype(jnp.bfloat16)
    cotan_table = jnp.concatenate([scaled, zero_row], axis=0)
    width = FF // N_TP

    def per_expert(inputs):
        index, w_gate, w_up, w_down = inputs
        rows = row_table[index]
        cotan = cotan_table[index]
        gate_part, up_part, slot_dots, gate_grad, up_grad, down_grad = expert_grads(rows, cotan, w_gate, w_up, w_down)
        count = index.shape[0]
        parts_gate = gate_part.reshape(count, N_TP, width).transpose(1, 0, 2)
        parts_up = up_part.reshape(count, N_TP, width).transpose(1, 0, 2)
        split_gate = w_gate.reshape(D, N_TP, width).transpose(1, 0, 2)
        split_up = w_up.reshape(D, N_TP, width).transpose(1, 0, 2)

        def add_slice(total, pieces):
            piece_gate, piece_up, weight_gate, weight_up = pieces
            term = jnp.dot(piece_gate, weight_gate.T, preferred_element_type=jnp.float32)
            term = term + jnp.dot(piece_up, weight_up.T, preferred_element_type=jnp.float32)
            rounded = lax.optimization_barrier(term.astype(jnp.bfloat16))
            return total + rounded.astype(jnp.float32), None

        row_grad, _ = lax.scan(add_slice, jnp.zeros((count, D), jnp.float32),
                               (parts_gate, parts_up, split_gate, split_up))
        return gate_grad, up_grad, down_grad, row_grad, slot_dots

    gate_grads, up_grads, down_grads, row_grads, dots = lax.map(
        per_expert, (owner, gate_weight, up_weight, down_weight))
    targets = owner.reshape(-1)
    slot_grad = jnp.zeros((slot_count + 1, D), jnp.float32).at[targets].add(row_grads.reshape(-1, D))
    tokens_grad = jnp.sum(slot_grad[:slot_count].reshape(TOKENS, TOPK, D), axis=1).astype(jnp.bfloat16)
    slot_dot = jnp.zeros((slot_count + 1,), jnp.float32).at[targets].add(dots.reshape(-1))
    gates_grad = slot_dot[:slot_count].reshape(TOKENS, TOPK) / gates
    return tokens_grad, gates_grad, gate_grads, up_grads, down_grads
```

```python
import functools

import jax
import jax.numpy as jnp
from jax import lax
from jax.experimental import pallas as pl
from jax.experimental.pallas import tpu as pltpu
from jax.sharding import PartitionSpec as P

MESH = pl.DeviceIdType.MESH
BF16 = jnp.bfloat16
F32 = jnp.float32
VMEM_BYTES = 60 * 1024 * 1024


def dot_nn(a, b):
    return lax.dot_general(a, b, (((1,), (0,)), ((), ())), preferred_element_type=F32)


def dot_nt(a, b):
    return lax.dot_general(a, b, (((1,), (1,)), ((), ())), preferred_element_type=F32)


def dot_tn(a, b):
    return lax.dot_general(a, b, (((0,), (0,)), ((), ())), preferred_element_type=F32)


def flip(t, bit):
    return t + bit - 2 * bit * lax.rem(lax.div(t, bit), 2)


def exchange_kernel(
    ep, tp, cap,
    tok_ref, og_ref, routes_ref, gates_ref, wg_hbm, wu_hbm, wd_hbm,
    tg_ref, gg_ref, xo_hbm, co_hbm, ho_hbm, gpo_hbm, upo_hbm,
    wg, wu, wd, sx, sc, xs, cs, comb_ref, dest_ref,
    pg, pu, hg, hid, gp, up,
    psib, rsib, pown, rown, mine, tsum, back, dsend, drecv, dsum, dback,
    wsem, osem,
    zs, zr, ns, nr, ds_, dr, ss, sr,
    bss, bsr, rs, rr, zbs, zbr, dts, dtr, dzs, dzr,
):
    me_e = lax.axis_index("ep")
    me_t = lax.axis_index("tp")
    sib = flip(me_t, 1)
    nbr = (flip(me_t, 2), flip(me_t, 4))
    diag = flip(nbr[0], 4)
    slots = ep * cap
    tok_dev, dw = tok_ref.shape
    fw = wg.shape[1]

    def rdma(src, dst, s_sem, r_sem, e, t):
        return pltpu.make_async_remote_copy(
            src_ref=src, dst_ref=dst, send_sem=s_sem, recv_sem=r_sem,
            device_id={"ep": e, "tp": t}, device_id_type=MESH,
        )

    loads = [
        pltpu.make_async_copy(src.at[0], dst, wsem.at[i])
        for i, (src, dst) in enumerate(((wg_hbm, wg), (wu_hbm, wu), (wd_hbm, wd)))
    ]
    for load in loads:
        load.start()

    barrier = pltpu.get_barrier_semaphore()
    for r in range(1, ep):
        pl.semaphore_signal(
            barrier, inc=1, device_id={"ep": lax.rem(me_e + r, ep), "tp": me_t}, device_id_type=MESH)
    for r in range(1, tp):
        pl.semaphore_signal(
            barrier, inc=1, device_id={"ep": me_e, "tp": lax.rem(me_t + r, tp)}, device_id_type=MESH)

    expert = [routes_ref[:, k : k + 1].astype(F32) for k in range(2)]
    lane = lax.broadcasted_iota(jnp.int32, (tok_dev, 128), 1).astype(F32)
    oh = [jnp.where(expert[k] == lane, 1.0, 0.0) for k in range(2)]
    row_id = lax.broadcasted_iota(jnp.int32, (tok_dev, tok_dev), 0)
    col_id = lax.broadcasted_iota(jnp.int32, (tok_dev, tok_dev), 1)
    below = jnp.where(col_id < row_id, 1.0, 0.0).astype(BF16)
    before = dot_nn(below, (oh[0] + oh[1]).astype(BF16))
    rank = [
        jnp.sum(before * oh[0], axis=1, keepdims=True),
        jnp.sum((before + oh[0]) * oh[1], axis=1, keepdims=True),
    ]
    slot_id = lax.broadcasted_iota(jnp.int32, (tok_dev, slots), 1).astype(F32)
    dest = [expert[k] * float(cap) + rank[k] for k in range(2)]
    comb = [jnp.where(dest[k] == slot_id, 1.0, 0.0) for k in range(2)]
    both = (comb[0] + comb[1]).astype(BF16)
    comb_ref[...] = both
    for k in range(2):
        dest_ref[k] = jnp.broadcast_to(dest[k], (tok_dev, 128))
    sx[...] = dot_tn(both, tok_ref[...]).astype(BF16)
    og = og_ref[...].astype(F32)
    scaled = jnp.concatenate([(gates_ref[:, k : k + 1] * og).astype(BF16) for k in range(2)], axis=0)
    picks = jnp.concatenate([comb[0], comb[1]], axis=0).astype(BF16)
    sc[...] = dot_tn(picks, scaled).astype(BF16)

    pl.semaphore_wait(barrier, ep - 1 + tp - 1)

    def rows_of(s):
        return pl.ds(pl.multiple_of(s * cap, cap), cap)

    sent, big = (sx, sc), (xs, cs)
    src_of = [lax.rem(me_e + ep - r, ep) for r in range(ep)]
    n_chunk = 2 * ep
    sends = []

    def start(copy):
        copy.start()
        sends.append(copy)
        return copy

    z_copy = {}
    for a in range(2):
        for r in range(1, ep):
            to = lax.rem(me_e + r, ep)
            z_copy[a * ep + r] = start(rdma(
                sent[a].at[rows_of(to)], big[a].at[me_t, rows_of(me_e)],
                zs.at[a * ep + r], zr.at[a * ep + r], to, me_t))
    for a in range(2):
        big[a][me_t, rows_of(me_e), :] = sent[a][rows_of(me_e), :]

    n_copy, d_copy, s_copy = {}, {}, {}

    def chunk(i, t):
        return big[i // ep].at[t, rows_of(src_of[i % ep])]

    def to_sibling(i, kind, t):
        s_copy[i, kind] = start(rdma(
            chunk(i, t), chunk(i, t), ss.at[i * 4 + kind], sr.at[i * 4 + kind], me_e, sib))

    def stage_a(i):
        if i in z_copy:
            z_copy[i].wait_recv()
        for d in range(2):
            n_copy[i, d] = start(rdma(
                chunk(i, me_t), chunk(i, me_t), ns.at[i * 2 + d], nr.at[i * 2 + d], me_e, nbr[d]))
        to_sibling(i, 0, me_t)

    def stage_b(i):
        for d in range(2):
            n_copy[i, d].wait_recv()
            if i % 2 == d:
                d_copy[i] = start(rdma(
                    chunk(i, nbr[d]), chunk(i, nbr[d]), ds_.at[i], dr.at[i], me_e, nbr[1 - d]))
            to_sibling(i, 1 + d, nbr[d])

    def stage_c(i):
        d_copy[i].wait_recv()
        to_sibling(i, 3, diag)

    def settle(a):
        for i in range(a * ep, (a + 1) * ep):
            for kind in range(4):
                s_copy[i, kind].wait_recv()

    def first_half(lo, hi):
        @pl.loop(lo, hi)
        def _(j):
            part = pl.ds(pl.multiple_of(j * dw, dw), dw)
            x = xs[j]
            pg[...] += dot_nn(x, wg[part, :])
            pu[...] += dot_nn(x, wu[part, :])

    outs = []

    def put(src, dst, k):
        copy = pltpu.make_async_copy(src, dst, osem.at[k])
        copy.start()
        outs.append(copy)

    pg[...] = jnp.zeros_like(pg)
    pu[...] = jnp.zeros_like(pu)
    hg[...] = jnp.zeros_like(hg)
    for i in range(n_chunk + 2):
        if i < n_chunk:
            stage_a(i)
        if 1 <= i <= n_chunk:
            stage_b(i - 1)
        if i >= 2:
            stage_c(i - 2)
        late = i - (ep + 2)
        if late == 0:
            settle(0)
            put(xs, xo_hbm, 0)
            loads[0].wait()
            loads[1].wait()
        if late >= 0:
            first_half(late * tp // ep, (late + 1) * tp // ep)
    settle(1)
    put(cs, co_hbm, 1)
    loads[2].wait()

    @pl.loop(0, tp)
    def _(j):
        part = pl.ds(pl.multiple_of(j * dw, dw), dw)
        hg[...] += dot_nt(cs[j], wd[:, part])

    block = 16

    @pl.loop(0, slots // block)
    def _(b):
        at = pl.ds(pl.multiple_of(b * block, block), block)
        g, u, h = pg[at, :], pu[at, :], hg[at, :]
        sig = jax.nn.sigmoid(g)
        act = g * sig
        hidden = (act * u).astype(BF16)
        hid[at, :] = hidden
        gp[at, :] = (h * u * sig * (1.0 + g * (1.0 - sig))).astype(BF16)
        up[at, :] = (h * act).astype(BF16)
        pg[at, :] = hidden.astype(F32) * h

    put(hid, ho_hbm, 2)
    put(gp, gpo_hbm, 3)
    put(up, upo_hbm, 4)

    def piece(t):
        part = pl.ds(pl.multiple_of(t * dw, dw), dw)
        return dot_nt(gp[...], wg[part, :]) + dot_nt(up[...], wu[part, :])

    chips = (diag, nbr[0], nbr[1], me_t)
    b_copy = []
    for q in range(4):
        psib[q] = piece(flip(chips[q], 1)).astype(BF16)
        b_copy.append(start(rdma(psib.at[q], rsib.at[q], bss.at[q], bsr.at[q], me_e, sib)))
    for q in range(3):
        own = piece(chips[q])
        b_copy[q].wait_recv()
        pown[q] = (own + rsib[q].astype(F32)).astype(BF16)
    order = list(range(1, ep)) + [0]
    r_copy = {}
    for r in order:
        for q in range(3):
            at = rows_of(lax.rem(me_e + r, ep))
            r_copy[r, q] = start(rdma(
                pown.at[q, at], rown.at[q, at], rs.at[r * 3 + q], rr.at[r * 3 + q], me_e, chips[q]))

    ones = jnp.ones((8, fw), F32)
    for s in range(ep):
        dsend[s] = lax.dot_general(
            ones, pg[s * cap : (s + 1) * cap, :], (((1,), (1,)), ((), ())),
            precision=lax.Precision.HIGHEST, preferred_element_type=F32)
    t_copy = []
    for r in range(1, tp):
        t_copy.append(start(rdma(
            dsend, drecv.at[r - 1], dts.at[r - 1], dtr.at[r - 1], me_e, lax.rem(me_t + r, tp))))

    own = piece(me_t)
    b_copy[3].wait_recv()
    mine[...] = own + rsib[3].astype(F32)
    dots = dsend[...]
    for copy_index, copy in enumerate(t_copy):
        copy.wait_recv()
        dots = dots + drecv[copy_index]
    dsum[...] = dots
    dz_copy = []
    for r in range(1, ep):
        to = lax.rem(me_e + r, ep)
        dz_copy.append(start(rdma(
            dsum.at[to], dback.at[me_e], dzs.at[r - 1], dzr.at[r - 1], to, me_t)))
    dback[me_e] = dsum[me_e]

    zb_copy = []
    for r in order:
        to = lax.rem(me_e + r, ep)
        at = rows_of(to)
        total = mine[at, :]
        for q in range(3):
            r_copy[r, q].wait_recv()
            total = total + rown[q, at, :].astype(F32)
        tsum[at, :] = total.astype(BF16)
        if r:
            zb_copy.append(start(rdma(
                tsum.at[at], back.at[rows_of(me_e)], zbs.at[r - 1], zbr.at[r - 1], to, me_t)))
        else:
            back[at, :] = tsum[at, :]

    for copy in dz_copy:
        copy.wait_recv()
    share = tok_dev // tp
    first = pl.ds(pl.multiple_of(me_t * share, share), share)
    slot_lane = lax.broadcasted_iota(jnp.int32, (share, cap), 1).astype(F32)
    grads = []
    for k in range(2):
        want = dest_ref[k, first, 0:1]
        total = jnp.zeros((share, 1), F32)
        for s in range(ep):
            hit = want == slot_lane + float(s * cap)
            total = total + jnp.sum(
                jnp.where(hit, dback[s, 0:1, :].astype(BF16).astype(F32), 0.0), axis=1, keepdims=True)
        grads.append(total)
    gg_ref[...] = jnp.concatenate(grads, axis=1) / gates_ref[first, :]

    for copy in zb_copy:
        copy.wait_recv()
    tg_ref[...] = dot_nn(comb_ref[...], back[...]).astype(BF16)
    for copy in sends:
        copy.wait_send()
    for copy in outs:
        copy.wait()


def weight_kernel(x_ref, c_ref, hid_ref, gp_ref, up_ref, gg_ref, ug_ref, dg_ref):
    x = x_ref[...]
    gg_ref[...] = dot_tn(x, gp_ref[...]).astype(BF16)
    ug_ref[...] = dot_tn(x, up_ref[...]).astype(BF16)
    dg_ref[...] = dot_tn(hid_ref[...], c_ref[...]).astype(BF16)


def fused(tokens, out_grad, routes, gates, gate_weight, up_weight, down_weight):
    tok_dev, top_k = routes.shape
    ep = lax.axis_size("ep")
    tp = lax.axis_size("tp")
    cap = (3 * tok_dev + ep - 1) // ep
    slots = ep * cap
    dw = tokens.shape[1]
    model = gate_weight.shape[1]
    fw = gate_weight.shape[2]
    share = tok_dev // tp
    vmem = pl.BlockSpec(memory_space=pltpu.VMEM)
    any_ = pl.BlockSpec(memory_space=pl.ANY)
    dma = lambda n: pltpu.SemaphoreType.DMA((n,))
    wide = jax.ShapeDtypeStruct((tp, slots, dw), BF16)
    part = jax.ShapeDtypeStruct((slots, fw), BF16)
    flops = 10 * slots * model * fw
    tokens_grad, gates_grad, xs, cs, hid, gp, up = pl.pallas_call(
        functools.partial(exchange_kernel, ep, tp, cap),
        out_shape=(
            jax.ShapeDtypeStruct((tok_dev, dw), BF16),
            jax.ShapeDtypeStruct((share, top_k), F32),
            wide, wide, part, part, part,
        ),
        in_specs=[vmem] * 4 + [any_] * 3,
        out_specs=[vmem, vmem] + [any_] * 5,
        scratch_shapes=[
            pltpu.VMEM((model, fw), BF16),
            pltpu.VMEM((model, fw), BF16),
            pltpu.VMEM((fw, model), BF16),
            pltpu.VMEM((slots, dw), BF16),
            pltpu.VMEM((slots, dw), BF16),
            pltpu.VMEM((tp, slots, dw), BF16),
            pltpu.VMEM((tp, slots, dw), BF16),
            pltpu.VMEM((tok_dev, slots), BF16),
            pltpu.VMEM((2, tok_dev, 128), F32),
            pltpu.VMEM((slots, fw), F32),
            pltpu.VMEM((slots, fw), F32),
            pltpu.VMEM((slots, fw), F32),
            pltpu.VMEM((slots, fw), BF16),
            pltpu.VMEM((slots, fw), BF16),
            pltpu.VMEM((slots, fw), BF16),
            pltpu.VMEM((4, slots, dw), BF16),
            pltpu.VMEM((4, slots, dw), BF16),
            pltpu.VMEM((3, slots, dw), BF16),
            pltpu.VMEM((3, slots, dw), BF16),
            pltpu.VMEM((slots, dw), F32),
            pltpu.VMEM((slots, dw), BF16),
            pltpu.VMEM((slots, dw), BF16),
            pltpu.VMEM((ep, 8, cap), F32),
            pltpu.VMEM((tp - 1, ep, 8, cap), F32),
            pltpu.VMEM((ep, 8, cap), F32),
            pltpu.VMEM((ep, 8, cap), F32),
            dma(3), dma(5),
            dma(2 * ep), dma(2 * ep), dma(4 * ep), dma(4 * ep), dma(2 * ep), dma(2 * ep),
            dma(8 * ep), dma(8 * ep),
            dma(4), dma(4), dma(3 * ep), dma(3 * ep), dma(ep), dma(ep),
            dma(tp), dma(tp), dma(ep), dma(ep),
        ],
        compiler_params=pltpu.CompilerParams(
            collective_id=0, has_side_effects=True, vmem_limit_bytes=VMEM_BYTES),
        cost_estimate=pl.CostEstimate(flops=flops, bytes_accessed=6 * model * fw, transcendentals=0),
    )(tokens, out_grad, routes, gates, gate_weight, up_weight, down_weight)
    whole = pl.BlockSpec((slots, fw), lambda j: (0, 0))
    slab = pl.BlockSpec((None, slots, dw), lambda j: (j, 0, 0))
    tall = pl.BlockSpec((None, dw, fw), lambda j: (0, j, 0))
    gate_grad, up_grad, down_grad = pl.pallas_call(
        weight_kernel,
        grid=(tp,),
        out_shape=(
            jax.ShapeDtypeStruct((1, model, fw), BF16),
            jax.ShapeDtypeStruct((1, model, fw), BF16),
            jax.ShapeDtypeStruct((1, fw, model), BF16),
        ),
        in_specs=[slab, slab, whole, whole, whole],
        out_specs=[tall, tall, pl.BlockSpec((None, fw, dw), lambda j: (0, 0, j))],
        compiler_params=pltpu.CompilerParams(vmem_limit_bytes=VMEM_BYTES),
        cost_estimate=pl.CostEstimate(
            flops=6 * slots * model * fw, bytes_accessed=6 * model * fw, transcendentals=0),
    )(xs, cs, hid, gp, up)
    return (tokens_grad, gates_grad, gate_grad, up_grad, down_grad)


def fits_fused(ep, tp, tokens, routes, gate_weight):
    cap = (3 * routes.shape[0] + ep - 1) // ep
    return (
        tp == 8 and 2 <= ep <= 8 and tp % ep == 0 and cap % 16 == 0 and cap <= 128
        and tokens.shape[1] % 128 == 0 and routes.shape[1] == 2
        and routes.shape[0] % (8 * tp) == 0
        and gate_weight.shape[2] % 16 == 0
    )


def expert_grads(rows, cotan, w_gate, w_up, w_down):
    pre_gate = jnp.dot(rows, w_gate, preferred_element_type=jnp.float32)
    pre_up = jnp.dot(rows, w_up, preferred_element_type=jnp.float32)
    activated = jax.nn.silu(pre_gate)
    hidden = (activated * pre_up).astype(jnp.bfloat16)
    hid_grad = jnp.dot(cotan, w_down.T, preferred_element_type=jnp.float32)
    sigmoid_gate = jax.nn.sigmoid(pre_gate)
    gate_part = (hid_grad * pre_up * sigmoid_gate * (1.0 + pre_gate * (1.0 - sigmoid_gate))).astype(
        jnp.bfloat16
    )
    up_part = (hid_grad * activated).astype(jnp.bfloat16)
    slot_dots = jnp.sum(hidden.astype(jnp.float32) * hid_grad, axis=1)
    down_grad = jnp.dot(hidden.T, cotan, preferred_element_type=jnp.float32).astype(jnp.bfloat16)
    gate_grad = jnp.dot(rows.T, gate_part, preferred_element_type=jnp.float32).astype(jnp.bfloat16)
    up_grad = jnp.dot(rows.T, up_part, preferred_element_type=jnp.float32).astype(jnp.bfloat16)
    return (gate_part, up_part, slot_dots, gate_grad, up_grad, down_grad)


def on_device(tokens, out_grad, routes, gates, gate_weight, up_weight, down_weight):
    tok_dev, top_k = routes.shape
    ep_size = lax.axis_size("ep")
    tp_size = lax.axis_size("tp")
    if fits_fused(ep_size, tp_size, tokens, routes, gate_weight):
        return fused(tokens, out_grad, routes, gates, gate_weight, up_weight, down_weight)
    capacity = (3 * tok_dev + ep_size - 1) // ep_size
    buffer_rows = ep_size * capacity
    slice_width = tokens.shape[1]
    flat_expert = routes.reshape(-1)
    onehot = (flat_expert[:, None] == jnp.arange(ep_size, dtype=jnp.int32)[None, :]).astype(
        jnp.int32
    )
    slot_rank = jnp.sum((jnp.cumsum(onehot, axis=0) - onehot) * onehot, axis=1)
    slot_dest = flat_expert * capacity + slot_rank
    placed = jnp.arange(buffer_rows, dtype=jnp.int32)[:, None] == slot_dest[None, :]
    placed_float = placed.astype(jnp.float32)
    select = jnp.any(placed.reshape(buffer_rows, tok_dev, top_k), axis=2).astype(jnp.bfloat16)
    slot_gate = jnp.dot(placed_float, gates.reshape(-1), precision=lax.Precision.HIGHEST)
    sent_rows = jnp.dot(select, tokens, preferred_element_type=jnp.float32).astype(jnp.bfloat16)
    cotan_rows = jnp.dot(select, out_grad, preferred_element_type=jnp.float32)
    sent_cotan = (slot_gate[:, None] * cotan_rows).astype(jnp.bfloat16)
    recv_rows, recv_cotan = (
        lax.all_to_all(
            sent_rows.reshape(ep_size, capacity, slice_width),
            "ep",
            split_axis=0,
            concat_axis=0,
            tiled=True,
        ),
        lax.all_to_all(
            sent_cotan.reshape(ep_size, capacity, slice_width),
            "ep",
            split_axis=0,
            concat_axis=0,
            tiled=True,
        ),
    )
    whole_rows, whole_cotan = (
        lax.all_gather(recv_rows, "tp", axis=2, tiled=True),
        lax.all_gather(recv_cotan, "tp", axis=2, tiled=True),
    )
    model_width = whole_rows.shape[2]
    rows = whole_rows.reshape(buffer_rows, model_width)
    cotan = whole_cotan.reshape(buffer_rows, model_width)
    w_gate = gate_weight[0]
    w_up = up_weight[0]
    gate_part, up_part, slot_dots, gate_grad, up_grad, down_grad = expert_grads(
        rows, cotan, w_gate, w_up, down_weight[0]
    )
    partial_value = jnp.dot(gate_part, w_gate.T, preferred_element_type=jnp.float32)
    partial_value = (
        partial_value + jnp.dot(up_part, w_up.T, preferred_element_type=jnp.float32)
    ).astype(jnp.bfloat16)
    share = tok_dev // tp_size
    start = lax.axis_index("tp") * share
    summed = lax.psum(slot_dots, "tp")
    row_sums = lax.psum_scatter(
        partial_value.reshape(ep_size, capacity, model_width), "tp", scatter_dimension=2, tiled=True
    ).astype(jnp.float32)
    back_rows, back_dots = (
        lax.all_to_all(
            row_sums.astype(jnp.bfloat16), "ep", split_axis=0, concat_axis=0, tiled=True
        ).astype(row_sums.dtype),
        lax.all_to_all(
            summed.reshape(ep_size, capacity).astype(jnp.bfloat16),
            "ep",
            split_axis=0,
            concat_axis=0,
            tiled=True,
        ).astype(jnp.float32),
    )
    slot_rows = back_rows.reshape(buffer_rows, slice_width)[slot_dest]
    tokens_grad = jnp.sum(slot_rows.reshape(tok_dev, top_k, slice_width), axis=1).astype(
        jnp.bfloat16
    )
    token_dots = back_dots.reshape(buffer_rows)[slot_dest].reshape(tok_dev, top_k)
    own_dots = lax.dynamic_slice_in_dim(token_dots, start, share, 0)
    own_gates = lax.dynamic_slice_in_dim(gates, start, share, 0)
    gates_grad = own_dots / own_gates
    return (tokens_grad, gates_grad, gate_grad[None], up_grad[None], down_grad[None])


def solution(mesh):
    placed = (
        P("ep", "tp"),
        P("ep", "tp"),
        P("ep", None),
        P("ep", None),
        P("ep", None, "tp"),
        P("ep", None, "tp"),
        P("ep", "tp", None),
    )
    return jax.shard_map(
        on_device,
        mesh=mesh,
        in_specs=placed,
        out_specs=(
            P("ep", "tp"),
            P(("ep", "tp"), None),
            P("ep", None, "tp"),
            P("ep", None, "tp"),
            P("ep", "tp", None),
        ),
        check_vma=False,
    )
```

```python
import functools

import jax
import jax.numpy as jnp
from jax import lax
from jax.experimental import pallas as pl
from jax.experimental.pallas import tpu as pltpu
from jax.sharding import PartitionSpec as P

MESH = pl.DeviceIdType.MESH
BF16 = jnp.bfloat16
F32 = jnp.float32
VMEM_BYTES = 60 * 1024 * 1024


def dot_nn(a, b):
    return lax.dot_general(a, b, (((1,), (0,)), ((), ())), preferred_element_type=F32)


def dot_nt(a, b):
    return lax.dot_general(a, b, (((1,), (1,)), ((), ())), preferred_element_type=F32)


def dot_tn(a, b):
    return lax.dot_general(a, b, (((0,), (0,)), ((), ())), preferred_element_type=F32)


def flip(t, bit):
    return t + bit - 2 * bit * lax.rem(lax.div(t, bit), 2)


def exchange_kernel(
    ep, tp, cap,
    tok_ref, og_ref, routes_ref, gates_ref, wg_hbm, wu_hbm, wd_hbm,
    tg_ref, gg_ref, xo_hbm, co_hbm, ho_hbm, gpo_hbm, upo_hbm,
    wg, wu, wd, sx, sc, xs, cs, comb_ref, pick_ref,
    pg, pu, hg, hid, gp, up, hid_t, gp_t, up_t,
    psib, rsib, pown, rown, mine, tsum, back, dsend, drecv, dsum, dback,
    wsem, osem,
    zs, zr, ns, nr, ds_, dr, ss, sr,
    bss, bsr, rs, rr, zbs, zbr, dts, dtr, dzs, dzr,
):
    me_e = lax.axis_index("ep")
    me_t = lax.axis_index("tp")
    sib = flip(me_t, 1)
    nbr = (flip(me_t, 2), flip(me_t, 4))
    diag = flip(nbr[0], 4)
    slots = ep * cap
    tok_dev, dw = tok_ref.shape
    fw = wg.shape[0]

    def rdma(src, dst, s_sem, r_sem, e, t):
        return pltpu.make_async_remote_copy(
            src_ref=src, dst_ref=dst, send_sem=s_sem, recv_sem=r_sem,
            device_id={"ep": e, "tp": t}, device_id_type=MESH,
        )

    loads = [
        pltpu.make_async_copy(src.at[0], dst, wsem.at[i])
        for i, (src, dst) in enumerate(((wg_hbm, wg), (wu_hbm, wu), (wd_hbm, wd)))
    ]
    for load in loads:
        load.start()

    barrier = pltpu.get_barrier_semaphore()
    for r in range(1, ep):
        pl.semaphore_signal(
            barrier, inc=1, device_id={"ep": lax.rem(me_e + r, ep), "tp": me_t}, device_id_type=MESH)
    for r in range(1, tp):
        pl.semaphore_signal(
            barrier, inc=1, device_id={"ep": me_e, "tp": lax.rem(me_t + r, tp)}, device_id_type=MESH)

    expert = [routes_ref[k : k + 1, :].astype(F32) for k in range(2)]
    group = lax.broadcasted_iota(jnp.int32, (16, tok_dev), 0).astype(F32)
    oh = [jnp.where(expert[k] == group, 1.0, 0.0) for k in range(2)]
    row_id = lax.broadcasted_iota(jnp.int32, (tok_dev, tok_dev), 0)
    col_id = lax.broadcasted_iota(jnp.int32, (tok_dev, tok_dev), 1)
    above = jnp.where(row_id < col_id, 1.0, 0.0).astype(BF16)
    before = dot_nn((oh[0] + oh[1]).astype(BF16), above)
    rank = [
        jnp.sum(before * oh[0], axis=0, keepdims=True),
        jnp.sum((before + oh[0]) * oh[1], axis=0, keepdims=True),
    ]
    slot_id = lax.broadcasted_iota(jnp.int32, (slots, tok_dev), 0).astype(F32)
    slot_gate = jnp.zeros((slots, 1), F32)
    both = jnp.zeros((slots, tok_dev), F32)
    for k in range(2):
        pick = jnp.where(expert[k] * float(cap) + rank[k] == slot_id, 1.0, 0.0)
        pick_ref[k] = pick
        both = both + pick
        slot_gate = slot_gate + jnp.sum(pick * gates_ref[k : k + 1, :], axis=1, keepdims=True)
    select = both.astype(BF16)
    comb_ref[...] = select
    sx[...] = dot_nn(select, tok_ref[...]).astype(BF16)
    sc[...] = (slot_gate * dot_nn(select, og_ref[...])).astype(BF16)

    pl.semaphore_wait(barrier, ep - 1 + tp - 1)

    def rows_of(s):
        return pl.ds(pl.multiple_of(s * cap, cap), cap)

    sent, big = (sx, sc), (xs, cs)
    src_of = [lax.rem(me_e + ep - r, ep) for r in range(ep)]
    n_chunk = 2 * ep
    sends = []

    def start(copy):
        copy.start()
        sends.append(copy)
        return copy

    z_copy = {}
    for a in range(2):
        for r in range(1, ep):
            to = lax.rem(me_e + r, ep)
            z_copy[a * ep + r] = start(rdma(
                sent[a].at[rows_of(to)], big[a].at[me_t, rows_of(me_e)],
                zs.at[a * ep + r], zr.at[a * ep + r], to, me_t))
    for a in range(2):
        big[a][me_t, rows_of(me_e), :] = sent[a][rows_of(me_e), :]

    n_copy, d_copy, s_copy = {}, {}, {}

    def chunk(i, t):
        return big[i // ep].at[t, rows_of(src_of[i % ep])]

    def to_sibling(i, kind, t):
        s_copy[i, kind] = start(rdma(
            chunk(i, t), chunk(i, t), ss.at[i * 4 + kind], sr.at[i * 4 + kind], me_e, sib))

    def stage_a(i):
        if i in z_copy:
            z_copy[i].wait_recv()
        for d in range(2):
            n_copy[i, d] = start(rdma(
                chunk(i, me_t), chunk(i, me_t), ns.at[i * 2 + d], nr.at[i * 2 + d], me_e, nbr[d]))
        to_sibling(i, 0, me_t)

    def stage_b(i):
        for d in range(2):
            n_copy[i, d].wait_recv()
            if i % 2 == d:
                d_copy[i] = start(rdma(
                    chunk(i, nbr[d]), chunk(i, nbr[d]), ds_.at[i], dr.at[i], me_e, nbr[1 - d]))
            to_sibling(i, 1 + d, nbr[d])

    def stage_c(i):
        d_copy[i].wait_recv()
        to_sibling(i, 3, diag)

    def settle(a):
        for i in range(a * ep, (a + 1) * ep):
            for kind in range(4):
                s_copy[i, kind].wait_recv()

    def first_half(lo, hi):
        @pl.loop(lo, hi)
        def _(j):
            part = pl.ds(pl.multiple_of(j * dw, dw), dw)
            x = xs[j]
            pg[...] += dot_nt(x, wg[:, part])
            pu[...] += dot_nt(x, wu[:, part])

    outs = []

    def put(src, dst, k):
        copy = pltpu.make_async_copy(src, dst, osem.at[k])
        copy.start()
        outs.append(copy)

    pg[...] = jnp.zeros_like(pg)
    pu[...] = jnp.zeros_like(pu)
    hg[...] = jnp.zeros_like(hg)
    for i in range(n_chunk + 2):
        if i < n_chunk:
            stage_a(i)
        if 1 <= i <= n_chunk:
            stage_b(i - 1)
        if i >= 2:
            stage_c(i - 2)
        late = i - (ep + 2)
        if late == 0:
            settle(0)
            put(xs, xo_hbm, 0)
            loads[0].wait()
            loads[1].wait()
        if late >= 0:
            first_half(late * tp // ep, (late + 1) * tp // ep)
    settle(1)
    put(cs, co_hbm, 1)
    loads[2].wait()

    @pl.loop(0, tp)
    def _(j):
        part = pl.ds(pl.multiple_of(j * dw, dw), dw)
        hg[...] += dot_nt(cs[j], wd[:, part])

    block = 16

    @pl.loop(0, slots // block)
    def _(b):
        at = pl.ds(pl.multiple_of(b * block, block), block)
        g, u, h = pg[at, :], pu[at, :], hg[at, :]
        sig = jax.nn.sigmoid(g)
        act = g * sig
        hidden = (act * u).astype(BF16)
        hid[at, :] = hidden
        gp[at, :] = (h * u * sig * (1.0 + g * (1.0 - sig))).astype(BF16)
        up[at, :] = (h * act).astype(BF16)
        pg[at, :] = hidden.astype(F32) * h

    def piece(t):
        part = pl.ds(pl.multiple_of(t * dw, dw), dw)
        return dot_nn(gp[...], wg[:, part]) + dot_nn(up[...], wu[:, part])

    chips = (diag, nbr[0], nbr[1], me_t)
    b_copy = []
    for q in range(4):
        psib[q] = piece(flip(chips[q], 1)).astype(BF16)
        b_copy.append(start(rdma(psib.at[q], rsib.at[q], bss.at[q], bsr.at[q], me_e, sib)))
    for q in range(3):
        own = piece(chips[q])
        b_copy[q].wait_recv()
        pown[q] = (own + rsib[q].astype(F32)).astype(BF16)
    order = list(range(1, ep)) + [0]
    r_copy = {}
    for r in order:
        for q in range(3):
            at = rows_of(lax.rem(me_e + r, ep))
            r_copy[r, q] = start(rdma(
                pown.at[q, at], rown.at[q, at], rs.at[r * 3 + q], rr.at[r * 3 + q], me_e, chips[q]))

    ones = jnp.ones((8, fw), F32)
    for s in range(ep):
        dsend[s] = lax.dot_general(
            ones, pg[s * cap : (s + 1) * cap, :], (((1,), (1,)), ((), ())),
            precision=lax.Precision.HIGHEST, preferred_element_type=F32)
    t_copy = []
    for r in range(1, tp):
        t_copy.append(start(rdma(
            dsend, drecv.at[r - 1], dts.at[r - 1], dtr.at[r - 1], me_e, lax.rem(me_t + r, tp))))

    for k, (rows, flat, out) in enumerate(((hid, hid_t, ho_hbm), (gp, gp_t, gpo_hbm), (up, up_t, upo_hbm))):
        flat[...] = rows[...].T
        put(flat, out, 2 + k)

    own = piece(me_t)
    b_copy[3].wait_recv()
    mine[...] = own + rsib[3].astype(F32)
    dots = dsend[...]
    for copy_index, copy in enumerate(t_copy):
        copy.wait_recv()
        dots = dots + drecv[copy_index]
    dsum[...] = dots
    dz_copy = []
    for r in range(1, ep):
        to = lax.rem(me_e + r, ep)
        dz_copy.append(start(rdma(
            dsum.at[to], dback.at[me_e], dzs.at[r - 1], dzr.at[r - 1], to, me_t)))
    dback[me_e] = dsum[me_e]

    zb_copy = []
    for r in order:
        to = lax.rem(me_e + r, ep)
        at = rows_of(to)
        total = mine[at, :]
        for q in range(3):
            r_copy[r, q].wait_recv()
            total = total + rown[q, at, :].astype(F32)
        tsum[at, :] = total.astype(BF16)
        if r:
            zb_copy.append(start(rdma(
                tsum.at[at], back.at[rows_of(me_e)], zbs.at[r - 1], zbr.at[r - 1], to, me_t)))
        else:
            back[at, :] = tsum[at, :]

    for copy in dz_copy:
        copy.wait_recv()
    share = tok_dev // tp
    own_row = lax.broadcasted_iota(jnp.int32, (tok_dev, share), 0)
    own_col = lax.broadcasted_iota(jnp.int32, (tok_dev, share), 1) + me_t * share
    own_pick = jnp.where(own_row == own_col, 1.0, 0.0)
    exact = dict(precision=lax.Precision.HIGHEST, preferred_element_type=F32)
    grads = []
    for k in range(2):
        total = jnp.zeros((8, tok_dev), F32)
        for s in range(ep):
            total = total + jnp.dot(dback[s], pick_ref[k, s * cap : (s + 1) * cap, :], **exact)
        grads.append(total[0:1, :] / gates_ref[k : k + 1, :])
    shares = jnp.concatenate([*grads, jnp.zeros((6, tok_dev), F32)], axis=0)
    gg_ref[...] = jnp.dot(shares, own_pick, **exact)[0:2, :]

    for copy in zb_copy:
        copy.wait_recv()
    tg_ref[...] = dot_tn(comb_ref[...], back[...]).astype(BF16)
    for copy in sends:
        copy.wait_send()
    for copy in outs:
        copy.wait()


def weight_kernel(x_ref, c_ref, hid_ref, gp_ref, up_ref, gg_ref, ug_ref, dg_ref):
    x = x_ref[...]
    gg_ref[...] = dot_nn(gp_ref[...], x).astype(BF16)
    ug_ref[...] = dot_nn(up_ref[...], x).astype(BF16)
    dg_ref[...] = dot_nn(hid_ref[...], c_ref[...]).astype(BF16)


def fused(tokens, out_grad, routes, gates, gate_weight, up_weight, down_weight):
    tok_dev, top_k = routes.shape
    ep = lax.axis_size("ep")
    tp = lax.axis_size("tp")
    cap = (3 * tok_dev + ep - 1) // ep
    slots = ep * cap
    dw = tokens.shape[1]
    model = gate_weight.shape[1]
    fw = gate_weight.shape[2]
    share = tok_dev // tp
    vmem = pl.BlockSpec(memory_space=pltpu.VMEM)
    any_ = pl.BlockSpec(memory_space=pl.ANY)
    dma = lambda n: pltpu.SemaphoreType.DMA((n,))
    wide = jax.ShapeDtypeStruct((tp, slots, dw), BF16)
    part = jax.ShapeDtypeStruct((fw, slots), BF16)
    flops = 10 * slots * model * fw
    tokens_grad, gates_grad, xs, cs, hid, gp, up = pl.pallas_call(
        functools.partial(exchange_kernel, ep, tp, cap),
        out_shape=(
            jax.ShapeDtypeStruct((tok_dev, dw), BF16),
            jax.ShapeDtypeStruct((top_k, share), F32),
            wide, wide, part, part, part,
        ),
        in_specs=[vmem] * 4 + [any_] * 3,
        out_specs=[vmem, vmem] + [any_] * 5,
        scratch_shapes=[
            pltpu.VMEM((fw, model), BF16),
            pltpu.VMEM((fw, model), BF16),
            pltpu.VMEM((fw, model), BF16),
            pltpu.VMEM((slots, dw), BF16),
            pltpu.VMEM((slots, dw), BF16),
            pltpu.VMEM((tp, slots, dw), BF16),
            pltpu.VMEM((tp, slots, dw), BF16),
            pltpu.VMEM((slots, tok_dev), BF16),
            pltpu.VMEM((2, slots, tok_dev), F32),
            pltpu.VMEM((slots, fw), F32),
            pltpu.VMEM((slots, fw), F32),
            pltpu.VMEM((slots, fw), F32),
            pltpu.VMEM((slots, fw), BF16),
            pltpu.VMEM((slots, fw), BF16),
            pltpu.VMEM((slots, fw), BF16),
            pltpu.VMEM((fw, slots), BF16),
            pltpu.VMEM((fw, slots), BF16),
            pltpu.VMEM((fw, slots), BF16),
            pltpu.VMEM((4, slots, dw), BF16),
            pltpu.VMEM((4, slots, dw), BF16),
            pltpu.VMEM((3, slots, dw), BF16),
            pltpu.VMEM((3, slots, dw), BF16),
            pltpu.VMEM((slots, dw), F32),
            pltpu.VMEM((slots, dw), BF16),
            pltpu.VMEM((slots, dw), BF16),
            pltpu.VMEM((ep, 8, cap), F32),
            pltpu.VMEM((tp - 1, ep, 8, cap), F32),
            pltpu.VMEM((ep, 8, cap), F32),
            pltpu.VMEM((ep, 8, cap), F32),
            dma(3), dma(5),
            dma(2 * ep), dma(2 * ep), dma(4 * ep), dma(4 * ep), dma(2 * ep), dma(2 * ep),
            dma(8 * ep), dma(8 * ep),
            dma(4), dma(4), dma(3 * ep), dma(3 * ep), dma(ep), dma(ep),
            dma(tp), dma(tp), dma(ep), dma(ep),
        ],
        compiler_params=pltpu.CompilerParams(
            collective_id=0, has_side_effects=True, vmem_limit_bytes=VMEM_BYTES),
        cost_estimate=pl.CostEstimate(flops=flops, bytes_accessed=6 * model * fw, transcendentals=0),
    )(tokens, out_grad, routes.T, gates.T, jnp.swapaxes(gate_weight, 1, 2),
      jnp.swapaxes(up_weight, 1, 2), down_weight)
    whole = pl.BlockSpec((fw, slots), lambda j: (0, 0))
    slab = pl.BlockSpec((None, slots, dw), lambda j: (j, 0, 0))
    tall = pl.BlockSpec((None, fw, dw), lambda j: (0, 0, j))
    gate_grad, up_grad, down_grad = pl.pallas_call(
        weight_kernel,
        grid=(tp,),
        out_shape=(
            jax.ShapeDtypeStruct((1, fw, model), BF16),
            jax.ShapeDtypeStruct((1, fw, model), BF16),
            jax.ShapeDtypeStruct((1, fw, model), BF16),
        ),
        in_specs=[slab, slab, whole, whole, whole],
        out_specs=[tall, tall, tall],
        compiler_params=pltpu.CompilerParams(vmem_limit_bytes=VMEM_BYTES),
        cost_estimate=pl.CostEstimate(
            flops=6 * slots * model * fw, bytes_accessed=6 * model * fw, transcendentals=0),
    )(xs, cs, hid, gp, up)
    return (tokens_grad, gates_grad.T, jnp.swapaxes(gate_grad, 1, 2), jnp.swapaxes(up_grad, 1, 2), down_grad)


def fits_fused(ep, tp, tokens, routes, gate_weight):
    cap = (3 * routes.shape[0] + ep - 1) // ep
    return (
        tp == 8 and 2 <= ep <= 8 and tp % ep == 0 and cap % 16 == 0 and cap <= 128
        and tokens.shape[1] % 128 == 0 and routes.shape[1] == 2
        and routes.shape[0] % (8 * tp) == 0
        and gate_weight.shape[2] % 16 == 0
    )


def expert_grads(rows, cotan, w_gate, w_up, w_down):
    pre_gate = jnp.dot(rows, w_gate, preferred_element_type=jnp.float32)
    pre_up = jnp.dot(rows, w_up, preferred_element_type=jnp.float32)
    activated = jax.nn.silu(pre_gate)
    hidden = (activated * pre_up).astype(jnp.bfloat16)
    hid_grad = jnp.dot(cotan, w_down.T, preferred_element_type=jnp.float32)
    sigmoid_gate = jax.nn.sigmoid(pre_gate)
    gate_part = (hid_grad * pre_up * sigmoid_gate * (1.0 + pre_gate * (1.0 - sigmoid_gate))).astype(
        jnp.bfloat16
    )
    up_part = (hid_grad * activated).astype(jnp.bfloat16)
    slot_dots = jnp.sum(hidden.astype(jnp.float32) * hid_grad, axis=1)
    down_grad = jnp.dot(hidden.T, cotan, preferred_element_type=jnp.float32).astype(jnp.bfloat16)
    gate_grad = jnp.dot(rows.T, gate_part, preferred_element_type=jnp.float32).astype(jnp.bfloat16)
    up_grad = jnp.dot(rows.T, up_part, preferred_element_type=jnp.float32).astype(jnp.bfloat16)
    return (gate_part, up_part, slot_dots, gate_grad, up_grad, down_grad)


def on_device(tokens, out_grad, routes, gates, gate_weight, up_weight, down_weight):
    tok_dev, top_k = routes.shape
    ep_size = lax.axis_size("ep")
    tp_size = lax.axis_size("tp")
    if fits_fused(ep_size, tp_size, tokens, routes, gate_weight):
        return fused(tokens, out_grad, routes, gates, gate_weight, up_weight, down_weight)
    capacity = (3 * tok_dev + ep_size - 1) // ep_size
    buffer_rows = ep_size * capacity
    slice_width = tokens.shape[1]
    flat_expert = routes.reshape(-1)
    onehot = (flat_expert[:, None] == jnp.arange(ep_size, dtype=jnp.int32)[None, :]).astype(
        jnp.int32
    )
    slot_rank = jnp.sum((jnp.cumsum(onehot, axis=0) - onehot) * onehot, axis=1)
    slot_dest = flat_expert * capacity + slot_rank
    placed = jnp.arange(buffer_rows, dtype=jnp.int32)[:, None] == slot_dest[None, :]
    placed_float = placed.astype(jnp.float32)
    select = jnp.any(placed.reshape(buffer_rows, tok_dev, top_k), axis=2).astype(jnp.bfloat16)
    slot_gate = jnp.dot(placed_float, gates.reshape(-1), precision=lax.Precision.HIGHEST)
    sent_rows = jnp.dot(select, tokens, preferred_element_type=jnp.float32).astype(jnp.bfloat16)
    cotan_rows = jnp.dot(select, out_grad, preferred_element_type=jnp.float32)
    sent_cotan = (slot_gate[:, None] * cotan_rows).astype(jnp.bfloat16)
    recv_rows, recv_cotan = (
        lax.all_to_all(
            sent_rows.reshape(ep_size, capacity, slice_width),
            "ep",
            split_axis=0,
            concat_axis=0,
            tiled=True,
        ),
        lax.all_to_all(
            sent_cotan.reshape(ep_size, capacity, slice_width),
            "ep",
            split_axis=0,
            concat_axis=0,
            tiled=True,
        ),
    )
    whole_rows, whole_cotan = (
        lax.all_gather(recv_rows, "tp", axis=2, tiled=True),
        lax.all_gather(recv_cotan, "tp", axis=2, tiled=True),
    )
    model_width = whole_rows.shape[2]
    rows = whole_rows.reshape(buffer_rows, model_width)
    cotan = whole_cotan.reshape(buffer_rows, model_width)
    w_gate = gate_weight[0]
    w_up = up_weight[0]
    gate_part, up_part, slot_dots, gate_grad, up_grad, down_grad = expert_grads(
        rows, cotan, w_gate, w_up, down_weight[0]
    )
    partial_value = jnp.dot(gate_part, w_gate.T, preferred_element_type=jnp.float32)
    partial_value = (
        partial_value + jnp.dot(up_part, w_up.T, preferred_element_type=jnp.float32)
    ).astype(jnp.bfloat16)
    share = tok_dev // tp_size
    start = lax.axis_index("tp") * share
    summed = lax.psum(slot_dots, "tp")
    row_sums = lax.psum_scatter(
        partial_value.reshape(ep_size, capacity, model_width), "tp", scatter_dimension=2, tiled=True
    ).astype(jnp.float32)
    back_rows, back_dots = (
        lax.all_to_all(
            row_sums.astype(jnp.bfloat16), "ep", split_axis=0, concat_axis=0, tiled=True
        ).astype(row_sums.dtype),
        lax.all_to_all(
            summed.reshape(ep_size, capacity).astype(jnp.bfloat16),
            "ep",
            split_axis=0,
            concat_axis=0,
            tiled=True,
        ).astype(jnp.float32),
    )
    slot_rows = back_rows.reshape(buffer_rows, slice_width)[slot_dest]
    tokens_grad = jnp.sum(slot_rows.reshape(tok_dev, top_k, slice_width), axis=1).astype(
        jnp.bfloat16
    )
    token_dots = back_dots.reshape(buffer_rows)[slot_dest].reshape(tok_dev, top_k)
    own_dots = lax.dynamic_slice_in_dim(token_dots, start, share, 0)
    own_gates = lax.dynamic_slice_in_dim(gates, start, share, 0)
    gates_grad = own_dots / own_gates
    return (tokens_grad, gates_grad, gate_grad[None], up_grad[None], down_grad[None])


def solution(mesh):
    placed = (
        P("ep", "tp"),
        P("ep", "tp"),
        P("ep", None),
        P("ep", None),
        P("ep", None, "tp"),
        P("ep", None, "tp"),
        P("ep", "tp", None),
    )
    return jax.shard_map(
        on_device,
        mesh=mesh,
        in_specs=placed,
        out_specs=(
            P("ep", "tp"),
            P(("ep", "tp"), None),
            P("ep", None, "tp"),
            P("ep", None, "tp"),
            P("ep", "tp", None),
        ),
        check_vma=False,
    )
```

```python
import functools

import jax
import jax.numpy as jnp
from jax import lax
from jax.experimental import pallas as pl
from jax.experimental.pallas import tpu as pltpu
from jax.sharding import PartitionSpec as P

MESH = pl.DeviceIdType.MESH
BF16 = jnp.bfloat16
F32 = jnp.float32
VMEM_BYTES = 60 * 1024 * 1024


def dot_nn(a, b):
    return lax.dot_general(a, b, (((1,), (0,)), ((), ())), preferred_element_type=F32)


def dot_nt(a, b):
    return lax.dot_general(a, b, (((1,), (1,)), ((), ())), preferred_element_type=F32)


def dot_tn(a, b):
    return lax.dot_general(a, b, (((0,), (0,)), ((), ())), preferred_element_type=F32)


def flip(t, bit):
    return t + bit - 2 * bit * lax.rem(lax.div(t, bit), 2)


def exchange_kernel(
    ep, tp, cap,
    tok_ref, og_ref, routes_ref, gates_ref, wg_hbm, wu_hbm, wd_hbm,
    tg_ref, gg_ref, xo_hbm, co_hbm, ho_hbm, gpo_hbm, upo_hbm,
    wg, wu, wd, sx, sc, xs, cs, comb_ref, pick_ref,
    pg, pu, hg, hid, gp, up, hid_t, gp_t, up_t,
    psib, rsib, pown, rown, mine, tsum, back, dsend, drecv, dsum, dback,
    wsem, osem,
    zs, zr, ns, nr, ds_, dr, ss, sr,
    bss, bsr, rs, rr, zbs, zbr, dts, dtr, dzs, dzr,
):
    me_e = lax.axis_index("ep")
    me_t = lax.axis_index("tp")
    sib = flip(me_t, 1)
    nbr = (flip(me_t, 2), flip(me_t, 4))
    diag = flip(nbr[0], 4)
    slots = ep * cap
    tok_dev, dw = tok_ref.shape
    fw = wg.shape[0]

    def rdma(src, dst, s_sem, r_sem, e, t):
        return pltpu.make_async_remote_copy(
            src_ref=src, dst_ref=dst, send_sem=s_sem, recv_sem=r_sem,
            device_id={"ep": e, "tp": t}, device_id_type=MESH,
        )

    loads = [
        pltpu.make_async_copy(src.at[0], dst, wsem.at[i])
        for i, (src, dst) in enumerate(((wg_hbm, wg), (wu_hbm, wu), (wd_hbm, wd)))
    ]
    for load in loads:
        load.start()

    barrier = pltpu.get_barrier_semaphore()
    for r in range(1, ep):
        pl.semaphore_signal(
            barrier, inc=1, device_id={"ep": lax.rem(me_e + r, ep), "tp": me_t}, device_id_type=MESH)
    for r in range(1, tp):
        pl.semaphore_signal(
            barrier, inc=1, device_id={"ep": me_e, "tp": lax.rem(me_t + r, tp)}, device_id_type=MESH)

    expert = [routes_ref[k : k + 1, :].astype(F32) for k in range(2)]
    group = lax.broadcasted_iota(jnp.int32, (16, tok_dev), 0).astype(F32)
    oh = [jnp.where(expert[k] == group, 1.0, 0.0) for k in range(2)]
    row_id = lax.broadcasted_iota(jnp.int32, (tok_dev, tok_dev), 0)
    col_id = lax.broadcasted_iota(jnp.int32, (tok_dev, tok_dev), 1)
    above = jnp.where(row_id < col_id, 1.0, 0.0).astype(BF16)
    before = dot_nn((oh[0] + oh[1]).astype(BF16), above)
    rank = [
        jnp.sum(before * oh[0], axis=0, keepdims=True),
        jnp.sum((before + oh[0]) * oh[1], axis=0, keepdims=True),
    ]
    slot_id = lax.broadcasted_iota(jnp.int32, (slots, tok_dev), 0).astype(F32)
    slot_gate = jnp.zeros((slots, 1), F32)
    both = jnp.zeros((slots, tok_dev), F32)
    for k in range(2):
        pick = jnp.where(expert[k] * float(cap) + rank[k] == slot_id, 1.0, 0.0)
        pick_ref[k] = pick
        both = both + pick
        slot_gate = slot_gate + jnp.sum(pick * gates_ref[k : k + 1, :], axis=1, keepdims=True)
    select = both.astype(BF16)
    comb_ref[...] = select
    sx[...] = dot_nn(select, tok_ref[...]).astype(BF16)
    sc[...] = (slot_gate * dot_nn(select, og_ref[...])).astype(BF16)

    pl.semaphore_wait(barrier, ep - 1 + tp - 1)

    def rows_of(s):
        return pl.ds(pl.multiple_of(s * cap, cap), cap)

    sent, big = (sx, sc), (xs, cs)
    src_of = [lax.rem(me_e + ep - r, ep) for r in range(ep)]
    n_chunk = 2 * ep
    sends = []

    def start(copy):
        copy.start()
        sends.append(copy)
        return copy

    z_copy = {}
    for a in range(2):
        for r in range(1, ep):
            to = lax.rem(me_e + r, ep)
            z_copy[a * ep + r] = start(rdma(
                sent[a].at[rows_of(to)], big[a].at[me_t, rows_of(me_e)],
                zs.at[a * ep + r], zr.at[a * ep + r], to, me_t))
    for a in range(2):
        big[a][me_t, rows_of(me_e), :] = sent[a][rows_of(me_e), :]

    n_copy, d_copy, s_copy = {}, {}, {}

    def chunk(i, t):
        return big[i // ep].at[t, rows_of(src_of[i % ep])]

    def to_sibling(i, kind, t):
        s_copy[i, kind] = start(rdma(
            chunk(i, t), chunk(i, t), ss.at[i * 4 + kind], sr.at[i * 4 + kind], me_e, sib))

    def stage_a(i):
        if i in z_copy:
            z_copy[i].wait_recv()
        for d in range(2):
            n_copy[i, d] = start(rdma(
                chunk(i, me_t), chunk(i, me_t), ns.at[i * 2 + d], nr.at[i * 2 + d], me_e, nbr[d]))
        to_sibling(i, 0, me_t)

    def stage_b(i):
        for d in range(2):
            n_copy[i, d].wait_recv()
            if i % 2 == d:
                d_copy[i] = start(rdma(
                    chunk(i, nbr[d]), chunk(i, nbr[d]), ds_.at[i], dr.at[i], me_e, nbr[1 - d]))
            to_sibling(i, 1 + d, nbr[d])

    def stage_c(i):
        d_copy[i].wait_recv()
        to_sibling(i, 3, diag)

    def settle(a):
        for i in range(a * ep, (a + 1) * ep):
            for kind in range(4):
                s_copy[i, kind].wait_recv()

    def first_half(lo, hi):
        @pl.loop(lo, hi)
        def _(j):
            part = pl.ds(pl.multiple_of(j * dw, dw), dw)
            x = xs[j]
            pg[...] += dot_nt(x, wg[:, part])
            pu[...] += dot_nt(x, wu[:, part])

    outs = []

    def put(src, dst, k):
        copy = pltpu.make_async_copy(src, dst, osem.at[k])
        copy.start()
        outs.append(copy)

    pg[...] = jnp.zeros_like(pg)
    pu[...] = jnp.zeros_like(pu)
    hg[...] = jnp.zeros_like(hg)
    for i in range(n_chunk + 2):
        if i < n_chunk:
            stage_a(i)
        if 1 <= i <= n_chunk:
            stage_b(i - 1)
        if i >= 2:
            stage_c(i - 2)
        late = i - (ep + 2)
        if late == 0:
            settle(0)
            put(xs, xo_hbm, 0)
            loads[0].wait()
            loads[1].wait()
        if late >= 0:
            first_half(late * tp // ep, (late + 1) * tp // ep)
    settle(1)
    put(cs, co_hbm, 1)
    loads[2].wait()

    @pl.loop(0, tp)
    def _(j):
        part = pl.ds(pl.multiple_of(j * dw, dw), dw)
        hg[...] += dot_nt(cs[j], wd[:, part])

    block = 16

    @pl.loop(0, slots // block)
    def _(b):
        at = pl.ds(pl.multiple_of(b * block, block), block)
        g, u, h = pg[at, :], pu[at, :], hg[at, :]
        sig = jax.nn.sigmoid(g)
        act = g * sig
        hidden = (act * u).astype(BF16)
        hid[at, :] = hidden
        gp[at, :] = (h * u * sig * (1.0 + g * (1.0 - sig))).astype(BF16)
        up[at, :] = (h * act).astype(BF16)
        pg[at, :] = hidden.astype(F32) * h

    def piece(t):
        part = pl.ds(pl.multiple_of(t * dw, dw), dw)
        return dot_nn(gp[...], wg[:, part]) + dot_nn(up[...], wu[:, part])

    ones = jnp.ones((8, fw), F32)
    tile_row = lax.broadcasted_iota(jnp.int32, (8, 128), 0)
    tile = jnp.zeros((8, 128), F32)
    for s in range(ep):
        sums = lax.dot_general(
            ones, pg[s * cap : (s + 1) * cap, :], (((1,), (1,)), ((), ())),
            precision=lax.Precision.HIGHEST, preferred_element_type=F32)
        if cap < 128:
            sums = jnp.concatenate([sums, jnp.zeros((8, 128 - cap), F32)], axis=1)
        tile = jnp.where(tile_row == s, sums, tile)
    dsend[...] = tile
    t_copy = []
    for r in range(1, tp):
        t_copy.append(start(rdma(
            dsend, drecv.at[r - 1], dts.at[r - 1], dtr.at[r - 1], me_e, lax.rem(me_t + r, tp))))

    chips = (diag, nbr[0], nbr[1], me_t)
    b_copy = []
    for q in range(4):
        psib[q] = piece(flip(chips[q], 1)).astype(BF16)
        b_copy.append(start(rdma(psib.at[q], rsib.at[q], bss.at[q], bsr.at[q], me_e, sib)))
    for q in range(3):
        own = piece(chips[q])
        b_copy[q].wait_recv()
        pown[q] = (own + rsib[q].astype(F32)).astype(BF16)
    order = list(range(1, ep)) + [0]
    r_copy = {}
    for r in order:
        for q in range(3):
            at = rows_of(lax.rem(me_e + r, ep))
            r_copy[r, q] = start(rdma(
                pown.at[q, at], rown.at[q, at], rs.at[r * 3 + q], rr.at[r * 3 + q], me_e, chips[q]))

    dots = dsend[...]
    for copy_index, copy in enumerate(t_copy):
        copy.wait_recv()
        dots = dots + drecv[copy_index]
    dsum[...] = dots
    dz_copy = []
    for r in range(1, ep):
        to = lax.rem(me_e + r, ep)
        dz_copy.append(start(rdma(dsum, dback.at[me_e], dzs.at[r - 1], dzr.at[r - 1], to, me_t)))
    dback[me_e] = dots

    for k, (rows, flat, out) in enumerate(((hid, hid_t, ho_hbm), (gp, gp_t, gpo_hbm), (up, up_t, upo_hbm))):
        flat[...] = rows[...].T
        put(flat, out, 2 + k)

    own = piece(me_t)
    b_copy[3].wait_recv()
    mine[...] = own + rsib[3].astype(F32)
    zb_copy = []
    for r in order:
        to = lax.rem(me_e + r, ep)
        at = rows_of(to)
        total = mine[at, :]
        for q in range(3):
            r_copy[r, q].wait_recv()
            total = total + rown[q, at, :].astype(F32)
        tsum[at, :] = total.astype(BF16)
        if r:
            zb_copy.append(start(rdma(
                tsum.at[at], back.at[rows_of(me_e)], zbs.at[r - 1], zbr.at[r - 1], to, me_t)))
        else:
            back[at, :] = tsum[at, :]

    for copy in dz_copy:
        copy.wait_recv()
    share = tok_dev // tp
    own_row = lax.broadcasted_iota(jnp.int32, (tok_dev, share), 0)
    own_col = lax.broadcasted_iota(jnp.int32, (tok_dev, share), 1) + me_t * share
    own_pick = jnp.where(own_row == own_col, 1.0, 0.0)
    exact = dict(precision=lax.Precision.HIGHEST, preferred_element_type=F32)
    mine_row = lax.broadcasted_iota(jnp.int32, (8, 128), 0) == me_e
    grads = []
    for k in range(2):
        total = jnp.zeros((8, tok_dev), F32)
        for s in range(ep):
            held = jnp.where(mine_row, dback[s], 0.0)[:, 0:cap]
            total = total + jnp.dot(held, pick_ref[k, s * cap : (s + 1) * cap, :], **exact)
        grads.append(jnp.sum(total, axis=0, keepdims=True) / gates_ref[k : k + 1, :])
    shares = jnp.concatenate([*grads, jnp.zeros((6, tok_dev), F32)], axis=0)
    gg_ref[...] = jnp.dot(shares, own_pick, **exact)[0:2, :]

    for copy in zb_copy:
        copy.wait_recv()
    tg_ref[...] = dot_tn(comb_ref[...], back[...]).astype(BF16)
    for copy in sends:
        copy.wait_send()
    for copy in outs:
        copy.wait()


def weight_kernel(x_ref, c_ref, hid_ref, gp_ref, up_ref, gg_ref, ug_ref, dg_ref):
    x = x_ref[...]
    gg_ref[...] = dot_nn(gp_ref[...], x).astype(BF16)
    ug_ref[...] = dot_nn(up_ref[...], x).astype(BF16)
    dg_ref[...] = dot_nn(hid_ref[...], c_ref[...]).astype(BF16)


def fused(tokens, out_grad, routes, gates, gate_weight, up_weight, down_weight):
    tok_dev, top_k = routes.shape
    ep = lax.axis_size("ep")
    tp = lax.axis_size("tp")
    cap = (3 * tok_dev + ep - 1) // ep
    slots = ep * cap
    dw = tokens.shape[1]
    model = gate_weight.shape[1]
    fw = gate_weight.shape[2]
    share = tok_dev // tp
    vmem = pl.BlockSpec(memory_space=pltpu.VMEM)
    any_ = pl.BlockSpec(memory_space=pl.ANY)
    dma = lambda n: pltpu.SemaphoreType.DMA((n,))
    wide = jax.ShapeDtypeStruct((tp, slots, dw), BF16)
    part = jax.ShapeDtypeStruct((fw, slots), BF16)
    flops = 10 * slots * model * fw
    tokens_grad, gates_grad, xs, cs, hid, gp, up = pl.pallas_call(
        functools.partial(exchange_kernel, ep, tp, cap),
        out_shape=(
            jax.ShapeDtypeStruct((tok_dev, dw), BF16),
            jax.ShapeDtypeStruct((top_k, share), F32),
            wide, wide, part, part, part,
        ),
        in_specs=[vmem] * 4 + [any_] * 3,
        out_specs=[vmem, vmem] + [any_] * 5,
        scratch_shapes=[
            pltpu.VMEM((fw, model), BF16),
            pltpu.VMEM((fw, model), BF16),
            pltpu.VMEM((fw, model), BF16),
            pltpu.VMEM((slots, dw), BF16),
            pltpu.VMEM((slots, dw), BF16),
            pltpu.VMEM((tp, slots, dw), BF16),
            pltpu.VMEM((tp, slots, dw), BF16),
            pltpu.VMEM((slots, tok_dev), BF16),
            pltpu.VMEM((2, slots, tok_dev), F32),
            pltpu.VMEM((slots, fw), F32),
            pltpu.VMEM((slots, fw), F32),
            pltpu.VMEM((slots, fw), F32),
            pltpu.VMEM((slots, fw), BF16),
            pltpu.VMEM((slots, fw), BF16),
            pltpu.VMEM((slots, fw), BF16),
            pltpu.VMEM((fw, slots), BF16),
            pltpu.VMEM((fw, slots), BF16),
            pltpu.VMEM((fw, slots), BF16),
            pltpu.VMEM((4, slots, dw), BF16),
            pltpu.VMEM((4, slots, dw), BF16),
            pltpu.VMEM((3, slots, dw), BF16),
            pltpu.VMEM((3, slots, dw), BF16),
            pltpu.VMEM((slots, dw), F32),
            pltpu.VMEM((slots, dw), BF16),
            pltpu.VMEM((slots, dw), BF16),
            pltpu.VMEM((8, 128), F32),
            pltpu.VMEM((tp - 1, 8, 128), F32),
            pltpu.VMEM((8, 128), F32),
            pltpu.VMEM((ep, 8, 128), F32),
            dma(3), dma(5),
            dma(2 * ep), dma(2 * ep), dma(4 * ep), dma(4 * ep), dma(2 * ep), dma(2 * ep),
            dma(8 * ep), dma(8 * ep),
            dma(4), dma(4), dma(3 * ep), dma(3 * ep), dma(ep), dma(ep),
            dma(tp), dma(tp), dma(ep), dma(ep),
        ],
        compiler_params=pltpu.CompilerParams(
            collective_id=0, has_side_effects=True, vmem_limit_bytes=VMEM_BYTES),
        cost_estimate=pl.CostEstimate(flops=flops, bytes_accessed=6 * model * fw, transcendentals=0),
    )(tokens, out_grad, routes.T, gates.T, jnp.swapaxes(gate_weight, 1, 2),
      jnp.swapaxes(up_weight, 1, 2), down_weight)
    whole = pl.BlockSpec((fw, slots), lambda j: (0, 0))
    slab = pl.BlockSpec((None, slots, dw), lambda j: (j, 0, 0))
    tall = pl.BlockSpec((None, fw, dw), lambda j: (0, 0, j))
    gate_grad, up_grad, down_grad = pl.pallas_call(
        weight_kernel,
        grid=(tp,),
        out_shape=(
            jax.ShapeDtypeStruct((1, fw, model), BF16),
            jax.ShapeDtypeStruct((1, fw, model), BF16),
            jax.ShapeDtypeStruct((1, fw, model), BF16),
        ),
        in_specs=[slab, slab, whole, whole, whole],
        out_specs=[tall, tall, tall],
        compiler_params=pltpu.CompilerParams(vmem_limit_bytes=VMEM_BYTES),
        cost_estimate=pl.CostEstimate(
            flops=6 * slots * model * fw, bytes_accessed=6 * model * fw, transcendentals=0),
    )(xs, cs, hid, gp, up)
    return (tokens_grad, gates_grad.T, jnp.swapaxes(gate_grad, 1, 2), jnp.swapaxes(up_grad, 1, 2), down_grad)


def fits_fused(ep, tp, tokens, routes, gate_weight):
    cap = (3 * routes.shape[0] + ep - 1) // ep
    return (
        tp == 8 and 2 <= ep <= 8 and tp % ep == 0 and cap % 16 == 0 and cap <= 128
        and tokens.shape[1] % 128 == 0 and routes.shape[1] == 2
        and routes.shape[0] % (8 * tp) == 0
        and gate_weight.shape[2] % 16 == 0
    )


def expert_grads(rows, cotan, w_gate, w_up, w_down):
    pre_gate = jnp.dot(rows, w_gate, preferred_element_type=jnp.float32)
    pre_up = jnp.dot(rows, w_up, preferred_element_type=jnp.float32)
    activated = jax.nn.silu(pre_gate)
    hidden = (activated * pre_up).astype(jnp.bfloat16)
    hid_grad = jnp.dot(cotan, w_down.T, preferred_element_type=jnp.float32)
    sigmoid_gate = jax.nn.sigmoid(pre_gate)
    gate_part = (hid_grad * pre_up * sigmoid_gate * (1.0 + pre_gate * (1.0 - sigmoid_gate))).astype(
        jnp.bfloat16
    )
    up_part = (hid_grad * activated).astype(jnp.bfloat16)
    slot_dots = jnp.sum(hidden.astype(jnp.float32) * hid_grad, axis=1)
    down_grad = jnp.dot(hidden.T, cotan, preferred_element_type=jnp.float32).astype(jnp.bfloat16)
    gate_grad = jnp.dot(rows.T, gate_part, preferred_element_type=jnp.float32).astype(jnp.bfloat16)
    up_grad = jnp.dot(rows.T, up_part, preferred_element_type=jnp.float32).astype(jnp.bfloat16)
    return (gate_part, up_part, slot_dots, gate_grad, up_grad, down_grad)


def on_device(tokens, out_grad, routes, gates, gate_weight, up_weight, down_weight):
    tok_dev, top_k = routes.shape
    ep_size = lax.axis_size("ep")
    tp_size = lax.axis_size("tp")
    if fits_fused(ep_size, tp_size, tokens, routes, gate_weight):
        return fused(tokens, out_grad, routes, gates, gate_weight, up_weight, down_weight)
    capacity = (3 * tok_dev + ep_size - 1) // ep_size
    buffer_rows = ep_size * capacity
    slice_width = tokens.shape[1]
    flat_expert = routes.reshape(-1)
    onehot = (flat_expert[:, None] == jnp.arange(ep_size, dtype=jnp.int32)[None, :]).astype(
        jnp.int32
    )
    slot_rank = jnp.sum((jnp.cumsum(onehot, axis=0) - onehot) * onehot, axis=1)
    slot_dest = flat_expert * capacity + slot_rank
    placed = jnp.arange(buffer_rows, dtype=jnp.int32)[:, None] == slot_dest[None, :]
    placed_float = placed.astype(jnp.float32)
    select = jnp.any(placed.reshape(buffer_rows, tok_dev, top_k), axis=2).astype(jnp.bfloat16)
    slot_gate = jnp.dot(placed_float, gates.reshape(-1), precision=lax.Precision.HIGHEST)
    sent_rows = jnp.dot(select, tokens, preferred_element_type=jnp.float32).astype(jnp.bfloat16)
    cotan_rows = jnp.dot(select, out_grad, preferred_element_type=jnp.float32)
    sent_cotan = (slot_gate[:, None] * cotan_rows).astype(jnp.bfloat16)
    recv_rows, recv_cotan = (
        lax.all_to_all(
            sent_rows.reshape(ep_size, capacity, slice_width),
            "ep",
            split_axis=0,
            concat_axis=0,
            tiled=True,
        ),
        lax.all_to_all(
            sent_cotan.reshape(ep_size, capacity, slice_width),
            "ep",
            split_axis=0,
            concat_axis=0,
            tiled=True,
        ),
    )
    whole_rows, whole_cotan = (
        lax.all_gather(recv_rows, "tp", axis=2, tiled=True),
        lax.all_gather(recv_cotan, "tp", axis=2, tiled=True),
    )
    model_width = whole_rows.shape[2]
    rows = whole_rows.reshape(buffer_rows, model_width)
    cotan = whole_cotan.reshape(buffer_rows, model_width)
    w_gate = gate_weight[0]
    w_up = up_weight[0]
    gate_part, up_part, slot_dots, gate_grad, up_grad, down_grad = expert_grads(
        rows, cotan, w_gate, w_up, down_weight[0]
    )
    partial_value = jnp.dot(gate_part, w_gate.T, preferred_element_type=jnp.float32)
    partial_value = (
        partial_value + jnp.dot(up_part, w_up.T, preferred_element_type=jnp.float32)
    ).astype(jnp.bfloat16)
    share = tok_dev // tp_size
    start = lax.axis_index("tp") * share
    summed = lax.psum(slot_dots, "tp")
    row_sums = lax.psum_scatter(
        partial_value.reshape(ep_size, capacity, model_width), "tp", scatter_dimension=2, tiled=True
    ).astype(jnp.float32)
    back_rows, back_dots = (
        lax.all_to_all(
            row_sums.astype(jnp.bfloat16), "ep", split_axis=0, concat_axis=0, tiled=True
        ).astype(row_sums.dtype),
        lax.all_to_all(
            summed.reshape(ep_size, capacity).astype(jnp.bfloat16),
            "ep",
            split_axis=0,
            concat_axis=0,
            tiled=True,
        ).astype(jnp.float32),
    )
    slot_rows = back_rows.reshape(buffer_rows, slice_width)[slot_dest]
    tokens_grad = jnp.sum(slot_rows.reshape(tok_dev, top_k, slice_width), axis=1).astype(
        jnp.bfloat16
    )
    token_dots = back_dots.reshape(buffer_rows)[slot_dest].reshape(tok_dev, top_k)
    own_dots = lax.dynamic_slice_in_dim(token_dots, start, share, 0)
    own_gates = lax.dynamic_slice_in_dim(gates, start, share, 0)
    gates_grad = own_dots / own_gates
    return (tokens_grad, gates_grad, gate_grad[None], up_grad[None], down_grad[None])


def solution(mesh):
    placed = (
        P("ep", "tp"),
        P("ep", "tp"),
        P("ep", None),
        P("ep", None),
        P("ep", None, "tp"),
        P("ep", None, "tp"),
        P("ep", "tp", None),
    )
    return jax.shard_map(
        on_device,
        mesh=mesh,
        in_specs=placed,
        out_specs=(
            P("ep", "tp"),
            P(("ep", "tp"), None),
            P("ep", None, "tp"),
            P("ep", None, "tp"),
            P("ep", "tp", None),
        ),
        check_vma=False,
    )
```
